32 devices in a mesh: sp: 8 (over z, y), dp: 4 (over x, core).
Axes of the slice: x: 2, y: 2, z: 4, core: 2. Of those that a mesh axis runs over, the one named last changes fastest.
Arguments:
- hidden_in: bfloat16 [4, 1024, 2048], P('dp', 'sp'), may hold values from -6 to 6
- queries: bfloat16 [4, 1024, 1536], P('dp', 'sp'), may hold values from -64 to 64
- key_value_latent: bfloat16 [4, 1024, 512], P('dp', 'sp'), may hold values from -6 to 6
- keys_rope: bfloat16 [4, 1024, 32], P('dp', 'sp'), may hold values from -4 to 4
- latent_norm_gain: float32 [512], replicated, may hold values from 0.1 to 1.9
- latent_up_weight: bfloat16 [512, 2048], replicated, may hold values from -0.25 to 0.25
- attn_gain: float32 [1024], replicated, may hold values from 0.1 to 1.9
- out_proj: bfloat16 [1024, 2048], replicated, may hold values from -0.1875 to 0.1875
- norm1_gain: float32 [2048], replicated, may hold values from 0.1 to 1.9
- norm1_bias: float32 [2048], replicated, may hold values from -1.5 to 1.5
- expert_ids: int32 [4, 1024, 4], P('dp', 'sp'), may hold values from 0 to 31, all different within a row; in each aligned block of 128 rows (0 to 127, 128 to 255, ..., all dimensions but the last counted through in order) at most 24 rows name the same one
- route_weights: float32 [4, 1024, 4], P('dp', 'sp'), may hold values from 0.1 to 1
- gate_proj: bfloat16 [32, 2048, 512], P(('sp', 'dp')), may hold values from -0.125 to 0.125
- up_proj: bfloat16 [32, 2048, 512], P(('sp', 'dp')), may hold values from -0.125 to 0.125
- down_proj: bfloat16 [32, 512, 2048], P(('sp', 'dp')), may hold values from -0.25 to 0.25
- shared_gate: bfloat16 [2048, 512], replicated, may hold values from -0.125 to 0.125
- shared_up: bfloat16 [2048, 512], replicated, may hold values from -0.125 to 0.125
- shared_down: bfloat16 [512, 2048], replicated, may hold values from -0.25 to 0.25
- norm2_gain: float32 [2048], replicated, may hold values from 0.1 to 1.9
- norm2_bias: float32 [2048], replicated, may hold values from -1.5 to 1.5
Outputs:
- result: bfloat16 [4, 1024, 2048], P('dp', 'sp')
The draws below stay inside these ranges and needn't reach their ends.
Inputs may be any that keep to these rules, and one draw needn't show every extreme that they name: `expert_ids`: each row names 4 different experts. Among the rows of one device (aligned blocks of 128 rows), no expert is named more than 24 times, a bound that some block reaches.
All inputs are finite; a program needn't handle non-finite values.
Results may differ from the reference program's by a relative error of at most 0.01.
Values may be sent and summed in bfloat16 or wider, within the bound.
No kernel may reach another device: no remote copies, remote signals or barrier semaphores. Data moves between devices by JAX's collectives and lax.ppermute only.
A program may use at most 128 MiB of HBM per device.

```python
import math
import jax
import jax.numpy as jnp
import numpy as np
from jax import lax

D = 2048
ATTENTION_HEADS = 16
PLAIN_HEAD_WIDTH = 64
QK_ROPE = 32
VALUE_HEAD_WIDTH = 64
LATENT_WIDTH = 512
D_EXPERT = 512
D_SHARED = 512
TOP_K = 4
TOK_DEV = 128
SEQUENCE_LENGTH = 1024
BATCH_SEQUENCES = 4
D_ATTN = 1024
EXPERTS = 32
CAP = 24


def rope_base(key):
    inner = jax.random.fold_in(key, 71)
    return jnp.clip(jax.random.normal(inner, (BATCH_SEQUENCES, SEQUENCE_LENGTH, QK_ROPE), jnp.float32), -4.0, 4.0)


def draw_keys_rope(key, part):
    return rope_base(key).astype(jnp.bfloat16)


def draw_queries(key, part):
    head_width = PLAIN_HEAD_WIDTH + QK_ROPE
    inner = jax.random.fold_in(key, 13)
    base = jnp.clip(jax.random.normal(inner, (BATCH_SEQUENCES, SEQUENCE_LENGTH, ATTENTION_HEADS, head_width), jnp.float32), -6.0, 6.0)
    return base.reshape(BATCH_SEQUENCES, SEQUENCE_LENGTH, ATTENTION_HEADS * head_width).astype(jnp.bfloat16)


def steps_of(stream_key, shape, cuts, low, largest):
    loudness, own = 1.0, jax.random.fold_in(stream_key, 6)
    for dim, blocks in cuts:
        steps = jnp.exp(jax.random.uniform(jax.random.fold_in(own, dim), (blocks,), jnp.float32, low / len(cuts), largest / len(cuts)))
        loudness = loudness * jnp.repeat(steps, shape[dim] // blocks).reshape([-1 if axis == dim else 1 for axis in range(len(shape))])
    return loudness


def routed_block(rng, own, number, rows, amount, top, bound, slope):
    sequence = jax.random.permutation(rng, amount)
    heavy_load, common = shares(amount, rows * top, bound, slope, True), shares(amount, rows * top, bound, slope, False)
    places = jnp.arange(amount)

    def named(tallies, offset_by):
        used = int((tallies > 0).sum())
        fixed = max(1, used // 4)
        moved = fixed + (places - fixed + offset_by * (used - fixed)) % max(1, amount - fixed)
        return jnp.zeros((amount,), jnp.int32).at[sequence[jnp.where(places < fixed, places, moved)]].set(jnp.asarray(tallies, jnp.int32))

    tallies = jnp.where(number % 4 == 0, named(heavy_load, number // 4), named(common, number - number // 4 - 1))
    mixed = jax.random.permutation(jax.random.fold_in(own, 3), amount)
    source_of, sink = mixed[0:amount // 2 * 2:2], mixed[1:amount // 2 * 2:2]
    slack = jnp.minimum(tallies[source_of] - 1, bound - tallies[sink]) // 2
    slack = jnp.where((source_of == sequence[0]) | (sink == sequence[0]) | (tallies[sink] == 0), 0, jnp.maximum(slack, 0))
    moved = jax.random.randint(jax.random.fold_in(own, 4), (amount // 2,), 0, 1 << 20) % (slack + 1)
    tallies = tallies.at[source_of].add(-moved).at[sink].add(moved)
    labels = jnp.searchsorted(jnp.cumsum(tallies), jnp.arange(rows * top), side="right").astype(jnp.int32)
    grid = labels.reshape(top, rows).T
    grid = grid[jax.random.permutation(jax.random.fold_in(own, 1), rows)]
    offset_by = jax.random.randint(jax.random.fold_in(own, 2), (rows, 1), 0, top)
    return jnp.take_along_axis(grid, (jnp.arange(top)[None, :] + offset_by) % top, axis=1)


def shares(number_of, total, limit, slope, full):
    portions = [(1 << 20) // math.isqrt(rank ** slope) + 1 for rank in range(1, number_of + 1)]
    largest = limit if full else min(limit, max(-(-total // number_of), total * portions[0] // sum(portions)))
    least = 1 if total - largest >= number_of - 1 else 0
    counts, surplus = [largest] + [least] * (number_of - 1), total - largest - least * (number_of - 1)
    while surplus > 0:
        candidates = [i for i in range(1, number_of) if counts[i] < largest] or [i for i in range(1, number_of) if counts[i] < limit]
        whole, budget = sum([portions[i] for i in candidates]), surplus
        for i in candidates:
            more = min(limit - counts[i], max(1, budget * portions[i] // whole), surplus)
            counts[i] = counts[i] + more
            surplus = surplus - more
    return np.array(counts)


def scatter_about(stream_key, dims, width, reach, shards=(), kind=jnp.bfloat16):
    values = width * jax.random.normal(stream_key, dims, jnp.float32)
    if shards:
        values = values * steps_of(stream_key, dims, shards, -0.22, 0.18)
    return jnp.clip(values, -reach, reach).astype(kind)


def setup_inputs(seed: int = 0) -> dict:
    splits = jax.random.split(jax.random.key(seed), 21)
    hidden_in = scatter_about(splits[0], (BATCH_SEQUENCES, SEQUENCE_LENGTH, D), 1.0, 6.0, ((0, 4), (1, 8)))
    queries = draw_queries(jax.random.fold_in(splits[20], 71), 0)
    key_value_latent = scatter_about(splits[2], (BATCH_SEQUENCES, SEQUENCE_LENGTH, LATENT_WIDTH), 1.0, 6.0, ((0, 4), (1, 8)))
    keys_rope = draw_keys_rope(jax.random.fold_in(splits[20], 71), 0)
    latent_norm_gain = jnp.clip(1.0 + 0.18 * jax.random.normal(splits[4], (LATENT_WIDTH,), jnp.float32), 0.1, 1.9)
    latent_up_weight = scatter_about(splits[5], (LATENT_WIDTH, ATTENTION_HEADS * (PLAIN_HEAD_WIDTH + VALUE_HEAD_WIDTH)), LATENT_WIDTH ** -0.5, 0.25)
    attn_gain = jnp.clip(1.0 + 0.18 * jax.random.normal(splits[6], (D_ATTN,), jnp.float32), 0.1, 1.9)
    out_proj = scatter_about(splits[7], (D_ATTN, D), D_ATTN ** -0.5, 0.1875)
    norm1_gain = jnp.clip(1.0 + 0.18 * jax.random.normal(splits[8], (D,), jnp.float32), 0.1, 1.9)
    norm1_bias = scatter_about(splits[9], (D,), 0.3, 1.5, (), jnp.float32)
    expert_ids_keys = jax.random.split(jax.random.fold_in(splits[10], 1), BATCH_SEQUENCES * SEQUENCE_LENGTH // TOK_DEV)
    expert_ids_turns = jax.random.permutation(jax.random.fold_in(splits[10], 3), BATCH_SEQUENCES * SEQUENCE_LENGTH // TOK_DEV)
    expert_ids = jax.vmap(lambda own, number: routed_block(jax.random.fold_in(splits[10], 2), own, number, TOK_DEV, EXPERTS, TOP_K, CAP, 2))(expert_ids_keys, expert_ids_turns).reshape((BATCH_SEQUENCES, SEQUENCE_LENGTH, TOP_K))
    route_weights = jnp.clip(0.1 + 0.9 * jax.random.uniform(splits[11], (BATCH_SEQUENCES, SEQUENCE_LENGTH, TOP_K), jnp.float32) ** steps_of(splits[11], (BATCH_SEQUENCES, SEQUENCE_LENGTH, TOP_K), ((0, 4), (1, 8)), -0.2, 0.2), 0.1, 1.0)
    gate_proj = scatter_about(splits[12], (EXPERTS, D, D_EXPERT), D ** -0.5, 0.125, ((0, 32),))
    up_proj = scatter_about(splits[13], (EXPERTS, D, D_EXPERT), D ** -0.5, 0.125, ((0, 32),))
    down_proj = scatter_about(splits[14], (EXPERTS, D_EXPERT, D), D_EXPERT ** -0.5, 0.25, ((0, 32),))
    shared_gate = scatter_about(splits[15], (D, D_SHARED), D ** -0.5, 0.125)
    shared_up = scatter_about(splits[16], (D, D_SHARED), D ** -0.5, 0.125)
    shared_down = scatter_about(splits[17], (D_SHARED, D), D_SHARED ** -0.5, 0.25)
    norm2_gain = jnp.clip(1.0 + 0.18 * jax.random.normal(splits[18], (D,), jnp.float32), 0.1, 1.9)
    norm2_bias = scatter_about(splits[19], (D,), 0.3, 1.5, (), jnp.float32)
    return {"hidden_in": hidden_in, "queries": queries, "key_value_latent": key_value_latent, "keys_rope": keys_rope, "latent_norm_gain": latent_norm_gain, "latent_up_weight": latent_up_weight, "attn_gain": attn_gain, "out_proj": out_proj, "norm1_gain": norm1_gain, "norm1_bias": norm1_bias, "expert_ids": expert_ids, "route_weights": route_weights, "gate_proj": gate_proj, "up_proj": up_proj, "down_proj": down_proj, "shared_gate": shared_gate, "shared_up": shared_up, "shared_down": shared_down, "norm2_gain": norm2_gain, "norm2_bias": norm2_bias}


ALPHA = 2.0 ** 0.25
ROUTED = 2.5
THETA = 10000.0

def rms_scaled(values, scaling):
    widened = values.astype(jnp.float32)
    return widened * lax.rsqrt(lax.optimization_barrier(jnp.mean(widened * widened, axis=-1, keepdims=True)) + 1e-06) * scaling

def layer_norm(values, scaling, bias_add):
    centre = values - lax.optimization_barrier(jnp.mean(values, axis=-1, keepdims=True))
    spread = lax.optimization_barrier(jnp.mean(centre * centre, axis=-1, keepdims=True))
    return centre * lax.rsqrt(spread + 1e-05) * scaling + bias_add

def rotation_tables(positions, rot_width):
    frequency = THETA ** (-jnp.arange(0, rot_width, 2, dtype=jnp.float32) / rot_width)
    angles = positions.astype(jnp.float32)[:, None] * frequency[None, :]
    return (jnp.cos(angles), jnp.sin(angles))

def turn(values, cosine_table, sine_table):
    half_width = values.shape[-1] // 2
    first_half = values[..., :half_width]
    second_half = values[..., half_width:]
    return jnp.concatenate([first_half * cosine_table - second_half * sine_table, second_half * cosine_table + first_half * sine_table], axis=-1)

def attend(query, key_full, values):
    length = query.shape[0]
    span_rows = 512 if length % 512 == 0 else length
    block_count = length // span_rows
    blocks = query.reshape(block_count, span_rows, query.shape[1])
    key_pos = jnp.arange(length, dtype=jnp.int32)
    factor = 1.0 / math.sqrt(query.shape[1])

    def one_block(inputs):
        block_index, query_rows = inputs
        scores = jnp.dot(query_rows, key_full.T, preferred_element_type=jnp.float32) * factor
        query_pos = block_index * span_rows + jnp.arange(span_rows, dtype=jnp.int32)
        scores = jnp.where(key_pos[None, :] <= query_pos[:, None], scores, -jnp.inf)
        row_max = lax.optimization_barrier(jnp.max(scores, axis=-1, keepdims=True))
        weights = jnp.exp(scores - row_max)
        weights = (weights / lax.optimization_barrier(jnp.sum(weights, axis=-1, keepdims=True))).astype(jnp.bfloat16)
        return jnp.dot(weights, values, preferred_element_type=jnp.float32).astype(jnp.bfloat16)
    attended = lax.map(one_block, (jnp.arange(block_count, dtype=jnp.int32), blocks))
    return attended.reshape(length, values.shape[1])

def swiglu_rows(rows, gate_mat, up_mat, down_mat):
    gated = jnp.dot(rows, gate_mat, preferred_element_type=jnp.float32)
    lifted = jnp.dot(rows, up_mat, preferred_element_type=jnp.float32)
    inner = (jax.nn.silu(gated) * lifted).astype(jnp.bfloat16)
    return jnp.dot(inner, down_mat, preferred_element_type=jnp.float32)

def mixer_sequence(hidden_seq, query_seq, latent_seq, rope_seq, latent_norm_gain, latent_up_weight, attn_gain, out_proj, norm1_gain, norm1_bias):
    length = hidden_seq.shape[0]
    normed = rms_scaled(latent_seq, latent_norm_gain).astype(jnp.bfloat16)
    keys_values = jnp.dot(normed, latent_up_weight, preferred_element_type=jnp.float32).astype(jnp.bfloat16)
    keys_values = keys_values.reshape(length, ATTENTION_HEADS, PLAIN_HEAD_WIDTH + VALUE_HEAD_WIDTH)
    cosine_table, sine_table = rotation_tables(jnp.arange(length, dtype=jnp.int32), QK_ROPE)
    keys_turned = turn(rope_seq.astype(jnp.float32), cosine_table, sine_table).astype(jnp.bfloat16)
    query_heads = query_seq.reshape(length, ATTENTION_HEADS, PLAIN_HEAD_WIDTH + QK_ROPE)
    query_turned = turn(query_heads[..., PLAIN_HEAD_WIDTH:].astype(jnp.float32), cosine_table[:, None, :], sine_table[:, None, :]).astype(jnp.bfloat16)
    query_full = jnp.concatenate([query_heads[..., :PLAIN_HEAD_WIDTH], query_turned], axis=-1)
    key_full = jnp.concatenate([keys_values[..., :PLAIN_HEAD_WIDTH], jnp.broadcast_to(keys_turned[:, None, :], (length, ATTENTION_HEADS, QK_ROPE))], axis=-1)
    values_heads = keys_values[..., PLAIN_HEAD_WIDTH:]
    by_head = lax.map(lambda inputs: attend(inputs[0], inputs[1], inputs[2]), (jnp.moveaxis(query_full, 1, 0), jnp.moveaxis(key_full, 1, 0), jnp.moveaxis(values_heads, 1, 0)))
    attended = jnp.moveaxis(by_head, 0, 1).reshape(length, ATTENTION_HEADS * VALUE_HEAD_WIDTH)
    attn_normed = rms_scaled(attended, attn_gain).astype(jnp.bfloat16)
    mixed = jnp.dot(attn_normed, out_proj, preferred_element_type=jnp.float32)
    return layer_norm(ALPHA * hidden_seq.astype(jnp.float32) + mixed, norm1_gain, norm1_bias).astype(jnp.bfloat16)

def reference(hidden_in, queries, key_value_latent, keys_rope, latent_norm_gain, latent_up_weight, attn_gain, out_proj, norm1_gain, norm1_bias, expert_ids, route_weights, gate_proj, up_proj, down_proj, shared_gate, shared_up, shared_down, norm2_gain, norm2_bias):
    batch_count = hidden_in.shape[0]
    length = hidden_in.shape[1]
    firsts = [mixer_sequence(hidden_in[member], queries[member], key_value_latent[member], keys_rope[member], latent_norm_gain, latent_up_weight, attn_gain, out_proj, norm1_gain, norm1_bias) for member in range(batch_count)]
    first = jnp.concatenate(firsts, axis=0)
    total = first.shape[0]
    blocks = total // TOK_DEV
    entries = expert_ids.reshape(blocks, TOK_DEV * TOP_K).astype(jnp.int32)
    onehot = (entries[:, :, None] == jnp.arange(EXPERTS, dtype=jnp.int32)[None, None, :]).astype(jnp.int32)
    earlier = jnp.cumsum(onehot, axis=1).astype(jnp.int32) - onehot
    slots = lax.optimization_barrier(jnp.sum(earlier * onehot, axis=-1)).astype(jnp.int32)
    block_ids = jnp.arange(blocks, dtype=jnp.int32)[:, None]
    places = (entries * (blocks * CAP) + block_ids * CAP + slots).reshape(-1).astype(jnp.int32)
    owners = (jnp.arange(total * TOP_K, dtype=jnp.int32) // TOP_K).astype(jnp.int32)
    table = jnp.full((EXPERTS * blocks * CAP,), total, jnp.int32).at[places].set(owners)
    padded = jnp.concatenate([first, jnp.zeros((1, D), jnp.bfloat16)], axis=0)

    def expert_block(inputs):
        gate_mat, up_mat, down_mat, picks = inputs
        return swiglu_rows(padded[picks], gate_mat, up_mat, down_mat).astype(jnp.bfloat16)
    expert_out = lax.map(expert_block, (gate_proj, up_proj, down_proj, table.reshape(EXPERTS, blocks * CAP)))
    gathered = expert_out.reshape(EXPERTS * blocks * CAP, D)[places].reshape(total, TOP_K, D)
    weights = route_weights.reshape(total, TOP_K).astype(jnp.float32)
    gates = weights / lax.optimization_barrier(jnp.sum(weights, axis=-1, keepdims=True)) * ROUTED
    routed = jnp.zeros((total, D), jnp.float32)
    for column in range(TOP_K):
        routed = routed + gates[:, column:column + 1] * gathered[:, column].astype(jnp.float32)
    feed = routed + swiglu_rows(first, shared_gate, shared_up, shared_down)
    result = layer_norm(ALPHA * first.astype(jnp.float32) + feed, norm2_gain, norm2_bias).astype(jnp.bfloat16)
    return result.reshape(batch_count, length, D)
```

```python
import functools
import math

import jax
import jax.numpy as jnp
from jax import lax
from jax.experimental import pallas as pl
from jax.experimental.pallas import tpu as pltpu
from jax.sharding import PartitionSpec as P

D = 2048
ATTENTION_HEADS = 16
PLAIN_HEAD_WIDTH = 64
QK_ROPE = 32
VALUE_HEAD_WIDTH = 64
TOP_K = 4


ALPHA = 2.0**0.25
ROUTED = 2.5
THETA = 10000.0
LANES = 128
MASKED = -1e30


def rms_scaled(values, scaling):
    widened = values.astype(jnp.float32)
    return (
        widened * lax.rsqrt(jnp.mean(widened * widened, axis=-1, keepdims=True) + 1e-06) * scaling
    )


def layer_norm(values, scaling, bias_add):
    centre = values - jnp.mean(values, axis=-1, keepdims=True)
    spread = jnp.mean(centre * centre, axis=-1, keepdims=True)
    return centre * lax.rsqrt(spread + 1e-05) * scaling + bias_add


def rotation_tables(positions, rot_width):
    frequency = THETA ** (-jnp.arange(0, rot_width, 2, dtype=jnp.float32) / rot_width)
    angles = positions.astype(jnp.float32)[:, None] * frequency[None, :]
    return (jnp.cos(angles), jnp.sin(angles))


def turn(values, cosine_table, sine_table):
    half_width = values.shape[-1] // 2
    first_half = values[..., :half_width]
    second_half = values[..., half_width:]
    return jnp.concatenate(
        [
            first_half * cosine_table - second_half * sine_table,
            second_half * cosine_table + first_half * sine_table,
        ],
        axis=-1,
    )


def swiglu_rows(rows, gate_mat, up_mat, down_mat):
    gated = jnp.dot(rows, gate_mat, preferred_element_type=jnp.float32)
    lifted = jnp.dot(rows, up_mat, preferred_element_type=jnp.float32)
    inner = (jax.nn.silu(gated) * lifted).astype(jnp.bfloat16)
    return jnp.dot(inner, down_mat, preferred_element_type=jnp.float32)


def depth_of(seq_devices):
    bits = seq_devices.bit_length() - 1
    return 1 << ((bits + 1) // 2)


def hop(values, dist):
    count = lax.axis_size("sp")
    return lax.ppermute(values, "sp", [(i, i ^ dist) for i in range(count)])


def attention_kernel(
    blocks,
    latent_width,
    here_ref,
    query_ref,
    *refs,
):
    packed_refs = refs[:blocks]
    (
        up_ref,
        hidden_ref,
        attn_gain_ref,
        gain_ref,
        bias_ref,
        out_proj_ref,
        out_ref,
        latent,
        rope,
        attended,
        out_proj,
        sem,
    ) = refs[blocks:]
    step = pl.program_id(0)
    steps = pl.num_programs(0)
    rows = hidden_ref.shape[0]
    load = pltpu.make_async_copy(out_proj_ref, out_proj, sem)

    @pl.when(step == 0)
    def _():
        load.start()
        for j in range(blocks):
            latent[j * rows : (j + 1) * rows, :] = packed_refs[j][:, :latent_width]
            rope[j * rows : (j + 1) * rows, :] = packed_refs[j][:, latent_width:]

    pair = jnp.dot(latent[...], up_ref[...], preferred_element_type=jnp.float32).astype(
        jnp.bfloat16
    )
    here = here_ref[0]
    width = PLAIN_HEAD_WIDTH + VALUE_HEAD_WIDTH
    factor = math.log2(math.e) / math.sqrt(PLAIN_HEAD_WIDTH + QK_ROPE)
    causal = lax.broadcasted_iota(jnp.int32, (rows, rows), 1) <= lax.broadcasted_iota(
        jnp.int32, (rows, rows), 0
    )
    outs = []
    for head in range(2):
        head_kv = pair[:, head * width : (head + 1) * width]
        key_full = jnp.concatenate([head_kv, rope[...]], axis=1)
        scores = lax.dot_general(
            query_ref[head],
            key_full,
            (((1,), (1,)), ((), ())),
            preferred_element_type=jnp.float32,
        )
        parts = [jnp.where(causal, scores[:, :rows], MASKED)]
        for j in range(1, blocks):
            seen = (here ^ j) < here
            parts.append(jnp.where(seen, scores[:, j * rows : (j + 1) * rows], MASKED))
        scores = jnp.concatenate(parts, axis=1)
        row_max = jnp.max(scores, axis=1, keepdims=True)
        weights = jnp.exp2((scores - row_max) * factor)
        total = jnp.sum(weights, axis=1, keepdims=True)
        summed = jnp.dot(
            weights.astype(jnp.bfloat16), head_kv, preferred_element_type=jnp.float32
        )
        outs.append(summed / total)
    lane = lax.broadcasted_iota(jnp.int32, (rows, width), 1)
    attended[step] = jnp.where(
        lane < PLAIN_HEAD_WIDTH, pltpu.roll(outs[0], PLAIN_HEAD_WIDTH, 1), outs[1]
    ).astype(jnp.bfloat16)

    @pl.when(step == steps - 1)
    def _():
        load.wait()
        whole = jnp.concatenate([attended[i] for i in range(attended.shape[0])], axis=1)
        normed = rms_scaled(whole, attn_gain_ref[...]).astype(jnp.bfloat16)
        mixed = jnp.dot(normed, out_proj[...], preferred_element_type=jnp.float32)
        out_ref[...] = layer_norm(
            ALPHA * hidden_ref[...].astype(jnp.float32) + mixed, gain_ref[...], bias_ref[...]
        ).astype(jnp.bfloat16)


def attention_layer(
    here, query_full, packed, latent_up_weight, hidden, attn_gain, out_proj, gain, bias
):
    blocks = len(packed)
    heads, rows, key_width = query_full.shape
    latent_width = latent_up_weight.shape[0]
    width = PLAIN_HEAD_WIDTH + VALUE_HEAD_WIDTH
    whole = lambda array: pl.BlockSpec(array.shape, lambda i: (0,) * array.ndim)
    return pl.pallas_call(
        functools.partial(attention_kernel, blocks, latent_width),
        grid=(heads // 2,),
        in_specs=[
            pl.BlockSpec(memory_space=pltpu.SMEM),
            pl.BlockSpec((2, rows, key_width), lambda i: (i, 0, 0)),
            *[whole(p) for p in packed],
            pl.BlockSpec((latent_width, 2 * width), lambda i: (0, i)),
            whole(hidden),
            whole(attn_gain),
            whole(gain),
            whole(bias),
            pl.BlockSpec(memory_space=pltpu.HBM),
        ],
        out_specs=pl.BlockSpec(hidden.shape, lambda i: (0, 0)),
        out_shape=jax.ShapeDtypeStruct(hidden.shape, jnp.bfloat16),
        scratch_shapes=[
            pltpu.VMEM((blocks * rows, latent_width), jnp.bfloat16),
            pltpu.VMEM((blocks * rows, packed[0].shape[1] - latent_width), jnp.bfloat16),
            pltpu.VMEM((heads // 2, rows, 2 * VALUE_HEAD_WIDTH), jnp.bfloat16),
            pltpu.VMEM(out_proj.shape, jnp.bfloat16),
            pltpu.SemaphoreType.DMA,
        ],
        compiler_params=pltpu.CompilerParams(
            dimension_semantics=("arbitrary",), vmem_limit_bytes=32 << 20
        ),
        name="attention_layer",
    )(here, query_full, *packed, latent_up_weight, hidden, attn_gain, gain, bias, out_proj)


def per_device(
    hidden_in,
    queries,
    key_value_latent,
    keys_rope,
    latent_norm_gain,
    latent_up_weight,
    attn_gain,
    out_proj,
    norm1_gain,
    norm1_bias,
    expert_ids,
    route_weights,
    gate_proj,
    up_proj,
    down_proj,
    shared_gate,
    shared_up,
    shared_down,
    norm2_gain,
    norm2_bias,
):
    seq_devices = lax.axis_size("sp")
    depth = depth_of(seq_devices)
    across = seq_devices // depth
    tok_rows = hidden_in.shape[1]
    here = lax.axis_index("sp")

    normed = rms_scaled(key_value_latent[0], latent_norm_gain).astype(jnp.bfloat16)
    local_pos = here * tok_rows + jnp.arange(tok_rows, dtype=jnp.int32)
    cosine, sine = rotation_tables(local_pos, QK_ROPE)
    keys_turned = turn(keys_rope[0].astype(jnp.float32), cosine, sine).astype(jnp.bfloat16)
    packed = jnp.concatenate(
        [normed, keys_turned, jnp.zeros((tok_rows, LANES - QK_ROPE), jnp.bfloat16)], axis=1
    )
    gathered = [packed] + [None] * (seq_devices - 1)
    for dz in range(depth - 1, 0, -1):
        gathered[dz * across] = hop(packed, dz * across)
    for dy in range(1, across):
        gathered[dy] = hop(packed, dy)
    for dz in range(1, depth):
        for dy in range(1, across):
            gathered[dz * across + dy] = hop(gathered[dz * across], dy)

    query_heads = queries[0].reshape(tok_rows, ATTENTION_HEADS, PLAIN_HEAD_WIDTH + QK_ROPE)
    query_turned = turn(
        query_heads[..., PLAIN_HEAD_WIDTH:].astype(jnp.float32),
        cosine[:, None, :],
        sine[:, None, :],
    ).astype(jnp.bfloat16)
    gap = lambda count: jnp.zeros((tok_rows, ATTENTION_HEADS, count), jnp.bfloat16)
    query_full = jnp.concatenate(
        [
            query_heads[..., :PLAIN_HEAD_WIDTH],
            gap(VALUE_HEAD_WIDTH),
            query_turned,
            gap(LANES - QK_ROPE),
        ],
        axis=-1,
    )
    first = attention_layer(
        here.reshape(1).astype(jnp.int32),
        jnp.moveaxis(query_full, 1, 0),
        gathered,
        latent_up_weight,
        hidden_in[0],
        attn_gain[None],
        out_proj,
        norm1_gain[None],
        norm1_bias[None],
    )
    group = lax.axis_size("sp") * lax.axis_size("dp")
    capacity = (tok_rows * TOP_K * 3 + 2 * group - 1) // (2 * group)
    entries = expert_ids[0].reshape(-1)
    onehot = (entries[:, None] == jnp.arange(group, dtype=jnp.int32)[None, :]).astype(jnp.int32)
    earlier = jnp.cumsum(onehot, axis=0) - onehot
    slots = jnp.sum(earlier * onehot, axis=-1)
    places = (entries * capacity + slots).reshape(tok_rows, TOP_K)
    slot_ids = jnp.arange(group * capacity, dtype=jnp.int32)
    dispatch = jnp.any(places[None, :, :] == slot_ids[:, None, None], axis=-1).astype(jnp.bfloat16)
    outbound = jnp.dot(dispatch, first, preferred_element_type=jnp.float32).astype(jnp.bfloat16)
    arrived = lax.all_to_all(
        outbound.reshape(group, capacity, D), ("sp", "dp"), split_axis=0, concat_axis=0, tiled=True
    )
    flat_rows = arrived.reshape(group * capacity, D)
    produced = (
        swiglu_rows(flat_rows, gate_proj[0], up_proj[0], down_proj[0])
        .astype(jnp.bfloat16)
        .reshape(group, capacity, D)
    )
    returned = lax.all_to_all(produced, ("sp", "dp"), split_axis=0, concat_axis=0, tiled=True)
    returned_flat = returned.reshape(group * capacity, D)
    weights = route_weights[0]
    gates = weights / jnp.sum(weights, axis=-1, keepdims=True) * ROUTED
    routed = jnp.zeros((tok_rows, D), jnp.float32)
    for column in range(TOP_K):
        picker = (places[:, column : column + 1] == slot_ids[None, :]).astype(jnp.bfloat16)
        picked = jnp.dot(picker, returned_flat, preferred_element_type=jnp.float32)
        routed = routed + gates[:, column : column + 1] * picked
    feed = routed + swiglu_rows(first, shared_gate, shared_up, shared_down)
    result = layer_norm(ALPHA * first.astype(jnp.float32) + feed, norm2_gain, norm2_bias).astype(
        jnp.bfloat16
    )
    return result.reshape(1, tok_rows, D)


def solution(mesh):
    in_specs = (
        P("dp", "sp", None),
        P("dp", "sp", None),
        P("dp", "sp", None),
        P("dp", "sp", None),
        P(),
        P(),
        P(),
        P(),
        P(),
        P(),
        P("dp", "sp", None),
        P("dp", "sp", None),
        P(("sp", "dp"), None, None),
        P(("sp", "dp"), None, None),
        P(("sp", "dp"), None, None),
        P(),
        P(),
        P(),
        P(),
        P(),
    )
    out_specs = P("dp", "sp", None)
    return jax.shard_map(
        per_device, mesh=mesh, in_specs=in_specs, out_specs=out_specs, check_vma=False
    )
```

```python
import functools
import math

import jax
import jax.numpy as jnp
import numpy as np
from jax import lax
from jax.experimental import pallas as pl
from jax.experimental.pallas import tpu as pltpu
from jax.sharding import PartitionSpec as P

D = 2048
ATTENTION_HEADS = 16
PLAIN_HEAD_WIDTH = 64
QK_ROPE = 32
VALUE_HEAD_WIDTH = 64
TOP_K = 4


ALPHA = 2.0**0.25
ROUTED = 2.5
THETA = 10000.0
LANES = 128
MASKED = -1e30
ROPE_LANE = 64
TAG_LANE = ROPE_LANE + QK_ROPE
HEADS_STEP = 4
VMEM_LIMIT = 60 << 20


def rms_scaled(values, scaling):
    widened = values.astype(jnp.float32)
    return (
        widened * lax.rsqrt(jnp.mean(widened * widened, axis=-1, keepdims=True) + 1e-06) * scaling
    )


def layer_norm(values, scaling, bias_add):
    centre = values - jnp.mean(values, axis=-1, keepdims=True)
    spread = jnp.mean(centre * centre, axis=-1, keepdims=True)
    return centre * lax.rsqrt(spread + 1e-05) * scaling + bias_add


def rotation_table(positions, rot_width):
    frequency = np.float32(THETA) ** (-np.arange(0, rot_width, 2, dtype=np.float32) / rot_width)
    angles = np.arange(positions, dtype=np.float32)[:, None] * frequency[None, :]
    table = np.zeros((positions, LANES), np.float32)
    half = rot_width // 2
    for side, values in enumerate((np.cos(angles), np.sin(angles))):
        start = ROPE_LANE + side * rot_width
        table[:, start : start + rot_width] = np.concatenate([values, values], axis=1)
    table[:, ROPE_LANE + rot_width : ROPE_LANE + rot_width + half] *= -1.0
    return jnp.asarray(table)


def turned(tile, table):
    lane = lax.broadcasted_iota(jnp.int32, tile.shape, 1)
    inside = (lane >= ROPE_LANE) & (lane < ROPE_LANE + QK_ROPE)
    half = QK_ROPE // 2
    other = jnp.where(
        lane < ROPE_LANE + half, pltpu.roll(tile, LANES - half, 1), pltpu.roll(tile, half, 1)
    )
    return jnp.where(inside, tile * table + other * pltpu.roll(table, LANES - QK_ROPE, 1), 0.0)


def pack_kernel(here_ref, latent_ref, gain_ref, side_ref, table_ref, out_ref):
    width = latent_ref.shape[1]
    out_ref[:, :width] = rms_scaled(latent_ref[...], gain_ref[...]).astype(jnp.bfloat16)
    side = side_ref[...]
    lane = lax.broadcasted_iota(jnp.int32, side.shape, 1)
    inside = (lane >= ROPE_LANE) & (lane < ROPE_LANE + QK_ROPE)
    out_ref[:, width:] = jnp.where(inside, turned(side, table_ref[...]), side).astype(
        jnp.bfloat16
    )


def pack(here, latent, gain, side, table):
    rows, width = latent.shape
    whole = lambda array: pl.BlockSpec(array.shape, lambda i, here: (0,) * array.ndim)
    return pl.pallas_call(
        pack_kernel,
        grid_spec=pltpu.PrefetchScalarGridSpec(
            num_scalar_prefetch=1,
            grid=(1,),
            in_specs=[
                whole(latent),
                whole(gain),
                whole(side),
                pl.BlockSpec((rows, LANES), lambda i, here: (here[0], 0)),
            ],
            out_specs=pl.BlockSpec((rows, width + LANES), lambda i, here: (0, 0)),
        ),
        out_shape=jax.ShapeDtypeStruct((rows, width + LANES), jnp.bfloat16),
        compiler_params=pltpu.CompilerParams(vmem_limit_bytes=VMEM_LIMIT),
        name="pack",
    )(here, latent, gain, side, table)


def swiglu_rows(rows, gate_mat, up_mat, down_mat):
    gated = jnp.dot(rows, gate_mat, preferred_element_type=jnp.float32)
    lifted = jnp.dot(rows, up_mat, preferred_element_type=jnp.float32)
    inner = (jax.nn.silu(gated) * lifted).astype(jnp.bfloat16)
    return jnp.dot(inner, down_mat, preferred_element_type=jnp.float32)


def depth_of(seq_devices):
    bits = seq_devices.bit_length() - 1
    return 1 << ((bits + 1) // 2)


def send(values, dsp, ddp):
    count, side = lax.axis_size("sp"), lax.axis_size("dp")
    pairs = [
        (i * side + k, (i ^ dsp) * side + (k ^ ddp)) for i in range(count) for k in range(side)
    ]
    return lax.ppermute(values, ("sp", "dp"), pairs)


def attention_kernel(blocks, latent_width, here_ref, query_ref, table_ref, *refs):
    packed_refs = refs[:blocks]
    (
        up_ref,
        hidden_ref,
        attn_gain_ref,
        gain_ref,
        bias_ref,
        out_proj_ref,
        out_ref,
        latent,
        rope,
        attended,
        out_proj,
        sem,
    ) = refs[blocks:]
    step = pl.program_id(0)
    steps = pl.num_programs(0)
    rows = hidden_ref.shape[0]
    load = pltpu.make_async_copy(out_proj_ref, out_proj, sem)

    @pl.when(step == 0)
    def _():
        load.start()
        for j in range(blocks):
            latent[j * rows : (j + 1) * rows, :] = packed_refs[j][:, :latent_width]
            rope[j * rows : (j + 1) * rows, :] = packed_refs[j][:, latent_width:]

    key_values = jnp.dot(latent[...], up_ref[...], preferred_element_type=jnp.float32).astype(
        jnp.bfloat16
    )
    here = here_ref[0]
    width = PLAIN_HEAD_WIDTH + VALUE_HEAD_WIDTH
    key_width = PLAIN_HEAD_WIDTH + QK_ROPE
    factor = math.log2(math.e) / math.sqrt(key_width)
    causal = lax.broadcasted_iota(jnp.int32, (rows, rows), 1) <= lax.broadcasted_iota(
        jnp.int32, (rows, rows), 0
    )
    lane = lax.broadcasted_iota(jnp.int32, (rows, LANES), 1)
    query = query_ref[...].astype(jnp.float32)
    outs = []
    for head in range(HEADS_STEP):
        tile, offset = divmod(head * key_width, LANES)
        mine = query[:, tile * LANES : (tile + 1) * LANES]
        if offset:
            mine = pltpu.roll(mine, LANES - offset, 1)
        if offset + key_width > LANES:
            after = query[:, (tile + 1) * LANES : (tile + 2) * LANES]
            mine = jnp.where(lane < LANES - offset, mine, pltpu.roll(after, LANES - offset, 1))
        query_full = jnp.concatenate(
            [jnp.where(lane < PLAIN_HEAD_WIDTH, mine, 0.0), turned(mine, table_ref[...])], axis=1
        ).astype(jnp.bfloat16)
        head_kv = key_values[:, head * width : (head + 1) * width]
        key_full = jnp.concatenate([head_kv, rope[...]], axis=1)
        scores = lax.dot_general(
            query_full,
            key_full,
            (((1,), (1,)), ((), ())),
            preferred_element_type=jnp.float32,
        )
        parts = [jnp.where(causal, scores[:, :rows], MASKED)]
        for j in range(1, blocks):
            seen = (here ^ j) < here
            parts.append(jnp.where(seen, scores[:, j * rows : (j + 1) * rows], MASKED))
        scores = jnp.concatenate(parts, axis=1)
        row_max = jnp.max(scores, axis=1, keepdims=True)
        weights = jnp.exp2((scores - row_max) * factor)
        total = jnp.sum(weights, axis=1, keepdims=True)
        summed = jnp.dot(
            weights.astype(jnp.bfloat16), head_kv, preferred_element_type=jnp.float32
        )
        outs.append(summed / total)
    for pair in range(HEADS_STEP // 2):
        left, right = outs[2 * pair : 2 * pair + 2]
        attended[step * (HEADS_STEP // 2) + pair] = jnp.where(
            lane < VALUE_HEAD_WIDTH, pltpu.roll(left, VALUE_HEAD_WIDTH, 1), right
        ).astype(jnp.bfloat16)

    @pl.when(step == steps - 1)
    def _():
        load.wait()
        whole = jnp.concatenate([attended[i] for i in range(attended.shape[0])], axis=1)
        normed = rms_scaled(whole, attn_gain_ref[...]).astype(jnp.bfloat16)
        mixed = jnp.dot(normed, out_proj[...], preferred_element_type=jnp.float32)
        out_ref[...] = layer_norm(
            ALPHA * hidden_ref[...].astype(jnp.float32) + mixed, gain_ref[...], bias_ref[...]
        ).astype(jnp.bfloat16)


def attention_layer(
    here, queries, table, packed, latent_up_weight, hidden, attn_gain, out_proj, gain, bias
):
    blocks = len(packed)
    rows = queries.shape[0]
    latent_width = latent_up_weight.shape[0]
    width = PLAIN_HEAD_WIDTH + VALUE_HEAD_WIDTH
    heads = latent_up_weight.shape[1] // width
    whole = lambda array: pl.BlockSpec(array.shape, lambda i, here: (0,) * array.ndim)
    return pl.pallas_call(
        functools.partial(attention_kernel, blocks, latent_width),
        grid_spec=pltpu.PrefetchScalarGridSpec(
            num_scalar_prefetch=1,
            grid=(heads // HEADS_STEP,),
            in_specs=[
                pl.BlockSpec(
                    (rows, HEADS_STEP * (PLAIN_HEAD_WIDTH + QK_ROPE)), lambda i, here: (0, i)
                ),
                pl.BlockSpec((rows, LANES), lambda i, here: (here[0], 0)),
                *[whole(p) for p in packed],
                pl.BlockSpec((latent_width, HEADS_STEP * width), lambda i, here: (0, i)),
                whole(hidden),
                whole(attn_gain),
                whole(gain),
                whole(bias),
                pl.BlockSpec(memory_space=pltpu.HBM),
            ],
            out_specs=pl.BlockSpec(hidden.shape, lambda i, here: (0, 0)),
            scratch_shapes=[
                pltpu.VMEM((blocks * rows, latent_width), jnp.bfloat16),
                pltpu.VMEM((blocks * rows, LANES), jnp.bfloat16),
                pltpu.VMEM((heads // 2, rows, 2 * VALUE_HEAD_WIDTH), jnp.bfloat16),
                pltpu.VMEM(out_proj.shape, jnp.bfloat16),
                pltpu.SemaphoreType.DMA,
            ],
        ),
        out_shape=jax.ShapeDtypeStruct(hidden.shape, jnp.bfloat16),
        compiler_params=pltpu.CompilerParams(
            dimension_semantics=("arbitrary",), vmem_limit_bytes=VMEM_LIMIT
        ),
        name="attention_layer",
    )(here, queries, table, *packed, latent_up_weight, hidden, attn_gain, gain, bias, out_proj)


def per_device(
    hidden_in,
    queries,
    key_value_latent,
    keys_rope,
    latent_norm_gain,
    latent_up_weight,
    attn_gain,
    out_proj,
    norm1_gain,
    norm1_bias,
    expert_ids,
    route_weights,
    gate_proj,
    up_proj,
    down_proj,
    shared_gate,
    shared_up,
    shared_down,
    norm2_gain,
    norm2_bias,
):
    seq_devices = lax.axis_size("sp")
    depth = depth_of(seq_devices)
    across = seq_devices // depth
    tok_rows = hidden_in.shape[1]
    here = lax.axis_index("sp")

    index = here.reshape(1).astype(jnp.int32)
    table = rotation_table(seq_devices * tok_rows, QK_ROPE)

    gates = route_weights[0] / jnp.sum(route_weights[0], axis=-1, keepdims=True) * ROUTED
    side = jnp.concatenate(
        [
            jnp.zeros((tok_rows, ROPE_LANE), jnp.float32),
            keys_rope[0].astype(jnp.float32),
            expert_ids[0].astype(jnp.float32),
            gates,
            jnp.zeros((tok_rows, LANES - TAG_LANE - 2 * TOP_K), jnp.float32),
        ],
        axis=1,
    )
    packed = pack(index, key_value_latent[0], latent_norm_gain[None], side, table)
    gathered = [packed] + [None] * (seq_devices - 1)
    for dz in range(depth - 1, 0, -1):
        gathered[dz * across] = send(packed, dz * across, 0)
    for dy in range(1, across):
        gathered[dy] = send(packed, dy, 0)
    for dz in range(1, depth):
        for dy in range(1, across):
            gathered[dz * across + dy] = send(gathered[dz * across], dy, 0)

    first = attention_layer(
        index,
        queries[0],
        table,
        gathered,
        latent_up_weight,
        hidden_in[0],
        attn_gain[None],
        out_proj,
        norm1_gain[None],
        norm1_bias[None],
    )

    side_devices = lax.axis_size("dp")
    group = seq_devices * side_devices
    capacity = (tok_rows * TOP_K * 3 + 2 * group - 1) // (2 * group)
    half = seq_devices // 2
    offsets = [(d, k) for d in range(half) for k in range(0, side_devices, 2)]
    peers = len(offsets)
    column = lax.axis_index("dp")
    wanted = jnp.stack([(here ^ d) * side_devices + (column ^ k) for d, k in offsets]).astype(
        jnp.float32
    )
    start = key_value_latent.shape[2] + TAG_LANE
    tags = jnp.stack([gathered[c * half][:, start : start + 2 * TOP_K] for c in range(2)])
    tags = jnp.stack([tags, send(tags, 0, 1)], axis=1).astype(jnp.float32)
    named = tags[..., :TOP_K, None] == wanted
    member = jnp.any(named, axis=3)
    share = jnp.sum(jnp.where(named, tags[..., TOP_K:, None], 0.0), axis=3)
    order = jnp.arange(tok_rows)
    before = (order[:, None] > order[None, :]).astype(jnp.bfloat16)
    slot = jnp.einsum(
        "ts,jbsp->jbtp", before, member.astype(jnp.bfloat16), preferred_element_type=jnp.float32
    ).astype(jnp.int32)
    filled = member[..., None] & (slot[..., None] == jnp.arange(capacity, dtype=jnp.int32))
    same = jnp.eye(2, dtype=jnp.bool_)
    slots = peers * 2 * capacity
    picks = (
        (jnp.transpose(filled, (0, 3, 1, 4, 2))[:, :, :, :, None, :] & same[:, None, :, None])
        .reshape(2, slots, 2 * tok_rows)
        .astype(jnp.bfloat16)
    )
    gated = jnp.where(filled, share[..., None], 0.0)
    mixes = (
        jnp.where(same[:, None, None, :, None], gated[:, :, :, :, None, :], 0.0)
        .reshape(2, 2 * tok_rows, slots)
        .astype(jnp.bfloat16)
    )

    def exchange(values):
        values = values.reshape(peers, 2 * capacity, D)
        parts = [values[0]] + [send(values[o], *offsets[o]) for o in range(1, peers)]
        return jnp.concatenate(parts, axis=0)

    rows = [first, send(first, half, 0)]
    feed = swiglu_rows(first, shared_gate, shared_up, shared_down)
    for c in range(2):
        both = jnp.concatenate([rows[c], send(rows[c], 0, 1)], axis=0)
        outbound = jnp.dot(picks[c], both, preferred_element_type=jnp.float32)
        arrived = exchange(outbound.astype(jnp.bfloat16))
        produced = swiglu_rows(arrived, gate_proj[0], up_proj[0], down_proj[0])
        returned = exchange(produced.astype(jnp.bfloat16))
        part = jnp.dot(mixes[c], returned, preferred_element_type=jnp.float32)
        part = part[:tok_rows] + send(part[tok_rows:].astype(jnp.bfloat16), 0, 1).astype(
            jnp.float32
        )
        if c:
            part = send(part.astype(jnp.bfloat16), half, 0).astype(jnp.float32)
        feed = feed + part
    result = layer_norm(ALPHA * first.astype(jnp.float32) + feed, norm2_gain, norm2_bias).astype(
        jnp.bfloat16
    )
    return result.reshape(1, tok_rows, D)


def solution(mesh):
    in_specs = (
        P("dp", "sp", None),
        P("dp", "sp", None),
        P("dp", "sp", None),
        P("dp", "sp", None),
        P(),
        P(),
        P(),
        P(),
        P(),
        P(),
        P("dp", "sp", None),
        P("dp", "sp", None),
        P(("sp", "dp"), None, None),
        P(("sp", "dp"), None, None),
        P(("sp", "dp"), None, None),
        P(),
        P(),
        P(),
        P(),
        P(),
    )
    out_specs = P("dp", "sp", None)
    return jax.shard_map(
        per_device, mesh=mesh, in_specs=in_specs, out_specs=out_specs, check_vma=False
    )
```

```python
import functools
import math

import jax
import jax.numpy as jnp
import numpy as np
from jax import lax
from jax.experimental import pallas as pl
from jax.experimental.pallas import tpu as pltpu
from jax.sharding import PartitionSpec as P


D = 2048
PLAIN_HEAD_WIDTH = 64
QK_ROPE = 32
VALUE_HEAD_WIDTH = 64
TOP_K = 4


ALPHA = 2.0**0.25
ROUTED = 2.5
THETA = 10000.0
LANES = 128
MASKED = -1e30
ROPE_LANE = 64
TAG_LANE = ROPE_LANE + QK_ROPE
HEADS_STEP = 4
VMEM_LIMIT = 32 << 20
VMEM_WIDE = 60 << 20


def rms_scaled(values, scaling):
    widened = values.astype(jnp.float32)
    return (
        widened * lax.rsqrt(jnp.mean(widened * widened, axis=-1, keepdims=True) + 1e-06) * scaling
    )


def layer_norm(values, scaling, bias_add):
    centre = values - jnp.mean(values, axis=-1, keepdims=True)
    spread = jnp.mean(centre * centre, axis=-1, keepdims=True)
    return centre * lax.rsqrt(spread + 1e-05) * scaling + bias_add


def rotation_table(positions, rot_width):
    frequency = np.float32(THETA) ** (-np.arange(0, rot_width, 2, dtype=np.float32) / rot_width)
    angles = np.arange(positions, dtype=np.float32)[:, None] * frequency[None, :]
    table = np.zeros((positions, LANES), np.float32)
    half = rot_width // 2
    for side, values in enumerate((np.cos(angles), np.sin(angles))):
        start = ROPE_LANE + side * rot_width
        table[:, start : start + rot_width] = np.concatenate([values, values], axis=1)
    table[:, ROPE_LANE + rot_width : ROPE_LANE + rot_width + half] *= -1.0
    return jnp.asarray(table)


def turned(tile, table):
    lane = lax.broadcasted_iota(jnp.int32, tile.shape, 1)
    inside = (lane >= ROPE_LANE) & (lane < ROPE_LANE + QK_ROPE)
    half = QK_ROPE // 2
    other = jnp.where(
        lane < ROPE_LANE + half, pltpu.roll(tile, LANES - half, 1), pltpu.roll(tile, half, 1)
    )
    return jnp.where(inside, tile * table + other * pltpu.roll(table, LANES - QK_ROPE, 1), 0.0)


def pack_kernel(
    here_ref, latent_ref, gain_ref, rope_ref, ids_ref, weights_ref, table_ref, out_ref
):
    width = latent_ref.shape[1]
    rows = latent_ref.shape[0]
    out_ref[:, :width] = rms_scaled(latent_ref[...], gain_ref[...]).astype(jnp.bfloat16)
    weights = weights_ref[...]
    gates = weights / jnp.sum(weights, axis=0, keepdims=True) * ROUTED
    side = jnp.concatenate(
        [
            jnp.zeros((ROPE_LANE, rows), jnp.float32),
            rope_ref[...].astype(jnp.float32),
            ids_ref[...].astype(jnp.float32),
            gates,
            jnp.zeros((LANES - TAG_LANE - 2 * TOP_K, rows), jnp.float32),
        ],
        axis=0,
    ).T
    lane = lax.broadcasted_iota(jnp.int32, side.shape, 1)
    inside = (lane >= ROPE_LANE) & (lane < ROPE_LANE + QK_ROPE)
    out_ref[:, width:] = jnp.where(inside, turned(side, table_ref[...]), side).astype(
        jnp.bfloat16
    )


def pack(here, latent, gain, rope, ids, weights, table):
    rows, width = latent.shape
    whole = lambda array: pl.BlockSpec(array.shape, lambda i, here: (0,) * array.ndim)
    return pl.pallas_call(
        pack_kernel,
        grid_spec=pltpu.PrefetchScalarGridSpec(
            num_scalar_prefetch=1,
            grid=(1,),
            in_specs=[
                whole(latent),
                whole(gain),
                whole(rope),
                whole(ids),
                whole(weights),
                pl.BlockSpec((rows, LANES), lambda i, here: (here[0], 0)),
            ],
            out_specs=pl.BlockSpec((rows, width + LANES), lambda i, here: (0, 0)),
        ),
        out_shape=jax.ShapeDtypeStruct((rows, width + LANES), jnp.bfloat16),
        compiler_params=pltpu.CompilerParams(vmem_limit_bytes=VMEM_WIDE),
        name="pack",
    )(here, latent, gain, rope, ids, weights, table)


def pick_kernel(picks_ref, own_ref, other_ref, *out_refs):
    both = jnp.concatenate([own_ref[...], other_ref[...]], axis=0)
    sent = jnp.dot(picks_ref[...], both, preferred_element_type=jnp.float32).astype(jnp.bfloat16)
    step = out_refs[0].shape[0]
    for o, out_ref in enumerate(out_refs):
        out_ref[...] = sent[o * step : (o + 1) * step, :]


def pick(picks, own, other, peers):
    rows, width = picks.shape[0] // peers, own.shape[1]
    return pl.pallas_call(
        pick_kernel,
        out_shape=[jax.ShapeDtypeStruct((rows, width), jnp.bfloat16)] * peers,
        compiler_params=pltpu.CompilerParams(vmem_limit_bytes=VMEM_LIMIT),
        name="pick",
    )(picks, own, other)


def mix_kernel(mixes_ref, *refs):
    parts, (own_ref, other_ref) = refs[:-2], refs[-2:]
    whole = jnp.concatenate([p[...] for p in parts], axis=0)
    mixed = jnp.dot(mixes_ref[...], whole, preferred_element_type=jnp.float32)
    rows = own_ref.shape[0]
    own_ref[...] = mixed[:rows]
    other_ref[...] = mixed[rows:].astype(jnp.bfloat16)


def mix(mixes, parts):
    shape = (mixes.shape[0] // 2, parts[0].shape[1])
    return pl.pallas_call(
        mix_kernel,
        out_shape=[
            jax.ShapeDtypeStruct(shape, jnp.float32),
            jax.ShapeDtypeStruct(shape, jnp.bfloat16),
        ],
        compiler_params=pltpu.CompilerParams(vmem_limit_bytes=VMEM_LIMIT),
        name="mix",
    )(mixes, *parts)


def swiglu_kernel(count, after, scale, *refs):
    parts = refs[:count]
    gate_ref, up_ref, down_ref = refs[count : count + 3]
    outs, (held, total) = refs[count + 3 + after : -2], refs[-2:]
    step = pl.program_id(0)
    size = parts[0].shape[0]

    @pl.when(step == 0)
    def _():
        for o, part in enumerate(parts):
            held[o * size : (o + 1) * size, :] = part[...]
        if scale:
            total[...] = scale * held[...].astype(jnp.float32)
        else:
            total[...] = jnp.zeros_like(total)

    rows = held[...]
    gated = jnp.dot(rows, gate_ref[...], preferred_element_type=jnp.float32)
    lifted = jnp.dot(rows, up_ref[...], preferred_element_type=jnp.float32)
    inner = (gated / (1.0 + jnp.exp(-gated)) * lifted).astype(jnp.bfloat16)
    total[...] += jnp.dot(inner, down_ref[...], preferred_element_type=jnp.float32)

    @pl.when(step == pl.num_programs(0) - 1)
    def _():
        for o, out in enumerate(outs):
            out[...] = total[o * size : (o + 1) * size, :].astype(out.dtype)


def swiglu(parts, gate_mat, up_mat, down_mat, kind, after=(), scale=0.0):
    count, (size, width) = len(parts), parts[0].shape
    hidden = gate_mat.shape[-1]
    block = min(hidden, 256)
    lead = (None,) * (gate_mat.ndim - 2)
    zero = (0,) * len(lead)
    whole = pl.BlockSpec((size, width), lambda i: (0, 0))
    return pl.pallas_call(
        functools.partial(swiglu_kernel, count, len(after), scale),
        grid=(hidden // block,),
        in_specs=[whole] * count
        + [pl.BlockSpec((*lead, width, block), lambda i: (*zero, 0, i))] * 2
        + [pl.BlockSpec((*lead, block, width), lambda i: (*zero, i, 0))]
        + [pl.BlockSpec(memory_space=pl.ANY)] * len(after),
        out_specs=[whole] * count,
        out_shape=[jax.ShapeDtypeStruct((size, width), kind)] * count,
        scratch_shapes=[
            pltpu.VMEM((count * size, width), jnp.bfloat16),
            pltpu.VMEM((count * size, width), jnp.float32),
        ],
        compiler_params=pltpu.CompilerParams(
            dimension_semantics=("arbitrary",), vmem_limit_bytes=VMEM_LIMIT
        ),
        name="swiglu",
    )(*parts, gate_mat, up_mat, down_mat, *after)


def finish_kernel(feed_ref, own_ref, core_ref, far_ref, gain_ref, bias_ref, out_ref):
    feed = feed_ref[...] + own_ref[...] + core_ref[...].astype(jnp.float32)
    feed = feed + far_ref[...].astype(jnp.float32)
    out_ref[...] = layer_norm(feed, gain_ref[...], bias_ref[...]).astype(jnp.bfloat16)


def finish(feed, *args):
    return pl.pallas_call(
        finish_kernel,
        out_shape=jax.ShapeDtypeStruct(feed.shape, jnp.bfloat16),
        compiler_params=pltpu.CompilerParams(vmem_limit_bytes=VMEM_LIMIT),
        name="finish",
    )(feed, *args)


def depth_of(seq_devices):
    bits = seq_devices.bit_length() - 1
    return 1 << ((bits + 1) // 2)


def send(values, dsp, ddp):
    count, side = lax.axis_size("sp"), lax.axis_size("dp")
    pairs = [
        (i * side + k, (i ^ dsp) * side + (k ^ ddp)) for i in range(count) for k in range(side)
    ]
    return lax.ppermute(values, ("sp", "dp"), pairs)


def attention_kernel(blocks, after, latent_width, here_ref, query_ref, table_ref, *refs):
    packed_refs = refs[:blocks]
    (
        up_ref,
        hidden_ref,
        attn_gain_ref,
        gain_ref,
        bias_ref,
        out_proj_ref,
    ) = refs[blocks : blocks + 6]
    out_ref, latent, rope, attended, out_proj, sem = refs[blocks + 6 + after :]
    step = pl.program_id(0)
    steps = pl.num_programs(0)
    rows = hidden_ref.shape[0]
    load = pltpu.make_async_copy(out_proj_ref, out_proj, sem)

    @pl.when(step == 0)
    def _():
        load.start()
        for j in range(blocks):
            latent[j * rows : (j + 1) * rows, :] = packed_refs[j][:, :latent_width]
            rope[j * rows : (j + 1) * rows, :] = packed_refs[j][:, latent_width:]

    key_values = jnp.dot(latent[...], up_ref[...], preferred_element_type=jnp.float32).astype(
        jnp.bfloat16
    )
    here = here_ref[0]
    width = PLAIN_HEAD_WIDTH + VALUE_HEAD_WIDTH
    key_width = PLAIN_HEAD_WIDTH + QK_ROPE
    factor = math.log2(math.e) / math.sqrt(key_width)
    causal = lax.broadcasted_iota(jnp.int32, (rows, rows), 1) <= lax.broadcasted_iota(
        jnp.int32, (rows, rows), 0
    )
    lane = lax.broadcasted_iota(jnp.int32, (rows, LANES), 1)
    query = query_ref[...].astype(jnp.float32)
    outs = []
    for head in range(HEADS_STEP):
        tile, offset = divmod(head * key_width, LANES)
        mine = query[:, tile * LANES : (tile + 1) * LANES]
        if offset:
            mine = pltpu.roll(mine, LANES - offset, 1)
        if offset + key_width > LANES:
            after = query[:, (tile + 1) * LANES : (tile + 2) * LANES]
            mine = jnp.where(lane < LANES - offset, mine, pltpu.roll(after, LANES - offset, 1))
        query_full = jnp.concatenate(
            [jnp.where(lane < PLAIN_HEAD_WIDTH, mine, 0.0), turned(mine, table_ref[...])], axis=1
        ).astype(jnp.bfloat16)
        head_kv = key_values[:, head * width : (head + 1) * width]
        key_full = jnp.concatenate([head_kv, rope[...]], axis=1)
        scores = lax.dot_general(
            query_full,
            key_full,
            (((1,), (1,)), ((), ())),
            preferred_element_type=jnp.float32,
        )
        parts = [jnp.where(causal, scores[:, :rows], MASKED)]
        for j in range(1, blocks):
            seen = (here ^ j) < here
            parts.append(jnp.where(seen, scores[:, j * rows : (j + 1) * rows], MASKED))
        scores = jnp.concatenate(parts, axis=1)
        row_max = jnp.max(scores, axis=1, keepdims=True)
        weights = jnp.exp2((scores - row_max) * factor)
        total = jnp.sum(weights, axis=1, keepdims=True)
        summed = jnp.dot(
            weights.astype(jnp.bfloat16), head_kv, preferred_element_type=jnp.float32
        )
        outs.append(summed / total)
    for pair in range(HEADS_STEP // 2):
        left, right = outs[2 * pair : 2 * pair + 2]
        attended[step * (HEADS_STEP // 2) + pair] = jnp.where(
            lane < VALUE_HEAD_WIDTH, pltpu.roll(left, VALUE_HEAD_WIDTH, 1), right
        ).astype(jnp.bfloat16)

    @pl.when(step == steps - 1)
    def _():
        load.wait()
        whole = jnp.concatenate([attended[i] for i in range(attended.shape[0])], axis=1)
        normed = rms_scaled(whole, attn_gain_ref[...]).astype(jnp.bfloat16)
        mixed = jnp.dot(normed, out_proj[...], preferred_element_type=jnp.float32)
        out_ref[...] = layer_norm(
            ALPHA * hidden_ref[...].astype(jnp.float32) + mixed, gain_ref[...], bias_ref[...]
        ).astype(jnp.bfloat16)


def attention_layer(
    here, queries, table, packed, latent_up_weight, hidden, attn_gain, out_proj, gain, bias, after=()
):
    blocks = len(packed)
    rows = queries.shape[0]
    latent_width = latent_up_weight.shape[0]
    width = PLAIN_HEAD_WIDTH + VALUE_HEAD_WIDTH
    heads = latent_up_weight.shape[1] // width
    whole = lambda array: pl.BlockSpec(array.shape, lambda i, here: (0,) * array.ndim)
    return pl.pallas_call(
        functools.partial(attention_kernel, blocks, len(after), latent_width),
        grid_spec=pltpu.PrefetchScalarGridSpec(
            num_scalar_prefetch=1,
            grid=(heads // HEADS_STEP,),
            in_specs=[
                pl.BlockSpec(
                    (rows, HEADS_STEP * (PLAIN_HEAD_WIDTH + QK_ROPE)), lambda i, here: (0, i)
                ),
                pl.BlockSpec((rows, LANES), lambda i, here: (here[0], 0)),
                *[whole(p) for p in packed],
                pl.BlockSpec((latent_width, HEADS_STEP * width), lambda i, here: (0, i)),
                whole(hidden),
                whole(attn_gain),
                whole(gain),
                whole(bias),
                pl.BlockSpec(memory_space=pltpu.HBM),
                *[pl.BlockSpec(memory_space=pl.ANY)] * len(after),
            ],
            out_specs=pl.BlockSpec(hidden.shape, lambda i, here: (0, 0)),
            scratch_shapes=[
                pltpu.VMEM((blocks * rows, latent_width), jnp.bfloat16),
                pltpu.VMEM((blocks * rows, LANES), jnp.bfloat16),
                pltpu.VMEM((heads // 2, rows, 2 * VALUE_HEAD_WIDTH), jnp.bfloat16),
                pltpu.VMEM(out_proj.shape, jnp.bfloat16),
                pltpu.SemaphoreType.DMA,
            ],
        ),
        out_shape=jax.ShapeDtypeStruct(hidden.shape, jnp.bfloat16),
        compiler_params=pltpu.CompilerParams(
            dimension_semantics=("arbitrary",), vmem_limit_bytes=VMEM_WIDE
        ),
        name="attention_layer",
    )(here, queries, table, *packed, latent_up_weight, hidden, attn_gain, gain, bias, out_proj, *after)


def per_device(
    hidden_in,
    queries,
    key_value_latent,
    keys_rope,
    latent_norm_gain,
    latent_up_weight,
    attn_gain,
    out_proj,
    norm1_gain,
    norm1_bias,
    expert_ids,
    route_weights,
    gate_proj,
    up_proj,
    down_proj,
    shared_gate,
    shared_up,
    shared_down,
    norm2_gain,
    norm2_bias,
):
    seq_devices = lax.axis_size("sp")
    depth = depth_of(seq_devices)
    across = seq_devices // depth
    tok_rows = hidden_in.shape[1]
    here = lax.axis_index("sp")

    index = here.reshape(1).astype(jnp.int32)
    table = rotation_table(seq_devices * tok_rows, QK_ROPE)

    packed = pack(
        index,
        key_value_latent[0],
        latent_norm_gain[None],
        keys_rope[0].T,
        expert_ids[0].T,
        route_weights[0].T,
        table,
    )
    gathered = [packed] + [None] * (seq_devices - 1)
    for dz in range(depth - 1, 0, -1):
        gathered[dz * across] = send(packed, dz * across, 0)
    for dy in range(1, across):
        gathered[dy] = send(packed, dy, 0)
    for dz in range(1, depth):
        for dy in range(1, across):
            gathered[dz * across + dy] = send(gathered[dz * across], dy, 0)

    side_devices = lax.axis_size("dp")
    group = seq_devices * side_devices
    capacity = (tok_rows * TOP_K * 3 + 2 * group - 1) // (2 * group)
    capacity = -(-capacity // 8) * 8
    half = seq_devices // 2
    offsets = [(d, k) for d in range(half) for k in range(0, side_devices, 2)]
    offsets = offsets[:1] + offsets[:0:-1]
    peers = len(offsets)
    slots = peers * 2 * capacity
    column = lax.axis_index("dp")
    wanted = jnp.stack([(here ^ d) * side_devices + (column ^ k) for d, k in offsets]).astype(
        jnp.float32
    )
    order = jnp.arange(tok_rows)
    before = (order[:, None] > order[None, :]).astype(jnp.bfloat16)
    same = jnp.eye(2, dtype=jnp.bool_)
    start = key_value_latent.shape[2] + TAG_LANE

    def routes(block):
        tags = block[:, start : start + 2 * TOP_K]
        tags = jnp.stack([tags, send(tags, 0, 1)]).astype(jnp.float32)
        named = tags[..., :TOP_K, None] == wanted
        member = jnp.any(named, axis=2)
        share = jnp.sum(jnp.where(named, tags[..., TOP_K:, None], 0.0), axis=2)
        slot = jnp.einsum(
            "ts,bsp->btp", before, member.astype(jnp.bfloat16), preferred_element_type=jnp.float32
        ).astype(jnp.int32)
        filled = member[..., None] & (slot[..., None] == jnp.arange(capacity, dtype=jnp.int32))
        picks = (
            (jnp.transpose(filled, (2, 0, 3, 1))[:, :, :, None, :] & same[:, None, :, None])
            .reshape(slots, 2 * tok_rows)
            .astype(jnp.bfloat16)
        )
        gated = jnp.where(filled, share[..., None], 0.0)
        mixes = (
            jnp.where(same[:, None, None, :, None], gated[:, :, :, None, :], 0.0)
            .reshape(2 * tok_rows, slots)
            .astype(jnp.bfloat16)
        )
        return picks, mixes

    near_picks, near_mixes = routes(packed)
    far_picks, far_mixes = routes(gathered[half])

    first = attention_layer(
        index,
        queries[0],
        table,
        gathered,
        latent_up_weight,
        hidden_in[0],
        attn_gain[None],
        out_proj,
        norm1_gain[None],
        norm1_bias[None],
        (near_picks, far_picks, near_mixes, far_mixes),
    )

    def exchange(parts):
        return [parts[0]] + [send(parts[o], *offsets[o]) for o in range(1, peers)]

    experts = functools.partial(swiglu, gate_mat=gate_proj, up_mat=up_proj, down_mat=down_proj)
    far = send(first, half, 0)
    sibling = send(first, 0, 1)
    near_sent = pick(near_picks, first, sibling, peers)
    near = exchange(near_sent)
    (feed,) = swiglu(
        [first], shared_gate, shared_up, shared_down, jnp.float32, near_sent[:1], ALPHA
    )
    far_sibling = send(far, 0, 1)
    far_sent = pick(far_picks, far, far_sibling, peers)
    away = exchange(far_sent)
    near_done = experts(near, kind=jnp.bfloat16, after=(far_sent[1], feed))
    away_done = experts(away, kind=jnp.bfloat16, after=near_done[1:2])
    away_back = exchange(away_done)
    near_back = exchange(near_done)
    far_own, far_core = mix(far_mixes, away_back)
    far_core = send(far_core, 0, 1)
    far_sum = (far_own + far_core.astype(jnp.float32)).astype(jnp.bfloat16)
    far_sum = send(far_sum, half, 0)
    own, core = mix(near_mixes, near_back)
    core = send(core, 0, 1)
    result = finish(feed, own, core, far_sum, norm2_gain[None], norm2_bias[None])
    return result.reshape(1, tok_rows, D)


def solution(mesh):
    in_specs = (
        P("dp", "sp", None),
        P("dp", "sp", None),
        P("dp", "sp", None),
        P("dp", "sp", None),
        P(),
        P(),
        P(),
        P(),
        P(),
        P(),
        P("dp", "sp", None),
        P("dp", "sp", None),
        P(("sp", "dp"), None, None),
        P(("sp", "dp"), None, None),
        P(("sp", "dp"), None, None),
        P(),
        P(),
        P(),
        P(),
        P(),
    )
    out_specs = P("dp", "sp", None)
    return jax.shard_map(
        per_device, mesh=mesh, in_specs=in_specs, out_specs=out_specs, check_vma=False
    )
```

```python
import functools
import math

import jax
import jax.numpy as jnp
import numpy as np
from jax import lax
from jax.experimental import pallas as pl
from jax.experimental.pallas import tpu as pltpu
from jax.sharding import PartitionSpec as P


D = 2048
PLAIN_HEAD_WIDTH = 64
QK_ROPE = 32
VALUE_HEAD_WIDTH = 64
TOP_K = 4


ALPHA = 2.0**0.25
ROUTED = 2.5
THETA = 10000.0
LANES = 128
MASKED = -1e30
ROPE_LANE = 64
TAG_LANE = ROPE_LANE + QK_ROPE
HEADS_STEP = 4
VMEM_LIMIT = 32 << 20
VMEM_WIDE = 60 << 20


def rms_scaled(values, scaling):
    widened = values.astype(jnp.float32)
    return (
        widened * lax.rsqrt(jnp.mean(widened * widened, axis=-1, keepdims=True) + 1e-06) * scaling
    )


def layer_norm(values, scaling, bias_add):
    centre = values - jnp.mean(values, axis=-1, keepdims=True)
    spread = jnp.mean(centre * centre, axis=-1, keepdims=True)
    return centre * lax.rsqrt(spread + 1e-05) * scaling + bias_add


def rotation_table(positions, rot_width):
    frequency = np.float32(THETA) ** (-np.arange(0, rot_width, 2, dtype=np.float32) / rot_width)
    angles = np.arange(positions, dtype=np.float32)[:, None] * frequency[None, :]
    table = np.zeros((positions, LANES), np.float32)
    half = rot_width // 2
    for side, values in enumerate((np.cos(angles), np.sin(angles))):
        start = ROPE_LANE + side * rot_width
        table[:, start : start + rot_width] = np.concatenate([values, values], axis=1)
    table[:, ROPE_LANE + rot_width : ROPE_LANE + rot_width + half] *= -1.0
    return jnp.asarray(table)


def turned(tile, table):
    lane = lax.broadcasted_iota(jnp.int32, tile.shape, 1)
    inside = (lane >= ROPE_LANE) & (lane < ROPE_LANE + QK_ROPE)
    half = QK_ROPE // 2
    other = jnp.where(
        lane < ROPE_LANE + half, pltpu.roll(tile, LANES - half, 1), pltpu.roll(tile, half, 1)
    )
    return jnp.where(inside, tile * table + other * pltpu.roll(table, LANES - QK_ROPE, 1), 0.0)


def pack_kernel(
    here_ref, latent_ref, gain_ref, rope_ref, ids_ref, weights_ref, table_ref, out_ref
):
    width = latent_ref.shape[1]
    rows = latent_ref.shape[0]
    out_ref[:, :width] = rms_scaled(latent_ref[...], gain_ref[...]).astype(jnp.bfloat16)
    weights = weights_ref[...]
    gates = weights / jnp.sum(weights, axis=0, keepdims=True) * ROUTED
    side = jnp.concatenate(
        [
            jnp.zeros((ROPE_LANE, rows), jnp.float32),
            rope_ref[...].astype(jnp.float32),
            ids_ref[...].astype(jnp.float32),
            gates,
            jnp.zeros((LANES - TAG_LANE - 2 * TOP_K, rows), jnp.float32),
        ],
        axis=0,
    ).T
    lane = lax.broadcasted_iota(jnp.int32, side.shape, 1)
    inside = (lane >= ROPE_LANE) & (lane < ROPE_LANE + QK_ROPE)
    out_ref[:, width:] = jnp.where(inside, turned(side, table_ref[...]), side).astype(
        jnp.bfloat16
    )


def pack(here, latent, gain, rope, ids, weights, table):
    rows, width = latent.shape
    whole = lambda array: pl.BlockSpec(array.shape, lambda i, here: (0,) * array.ndim)
    return pl.pallas_call(
        pack_kernel,
        grid_spec=pltpu.PrefetchScalarGridSpec(
            num_scalar_prefetch=1,
            grid=(1,),
            in_specs=[
                whole(latent),
                whole(gain),
                whole(rope),
                whole(ids),
                whole(weights),
                pl.BlockSpec((rows, LANES), lambda i, here: (here[0], 0)),
            ],
            out_specs=pl.BlockSpec((rows, width + LANES), lambda i, here: (0, 0)),
        ),
        out_shape=jax.ShapeDtypeStruct((rows, width + LANES), jnp.bfloat16),
        compiler_params=pltpu.CompilerParams(vmem_limit_bytes=VMEM_WIDE),
        name="pack",
    )(here, latent, gain, rope, ids, weights, table)


def pick_kernel(picks_ref, own_ref, other_ref, *out_refs):
    both = jnp.concatenate([own_ref[...], other_ref[...]], axis=0)
    sent = jnp.dot(picks_ref[...], both, preferred_element_type=jnp.float32).astype(jnp.bfloat16)
    step = out_refs[0].shape[0]
    for o, out_ref in enumerate(out_refs):
        out_ref[...] = sent[o * step : (o + 1) * step, :]


def pick(picks, own, other, peers):
    rows, width = picks.shape[0] // peers, own.shape[1]
    return pl.pallas_call(
        pick_kernel,
        out_shape=[jax.ShapeDtypeStruct((rows, width), jnp.bfloat16)] * peers,
        compiler_params=pltpu.CompilerParams(vmem_limit_bytes=VMEM_LIMIT),
        name="pick",
    )(picks, own, other)


def mix_kernel(mixes_ref, *refs):
    parts, (own_ref, other_ref) = refs[:-2], refs[-2:]
    whole = jnp.concatenate([p[...] for p in parts], axis=0)
    mixed = jnp.dot(mixes_ref[...], whole, preferred_element_type=jnp.float32)
    rows = own_ref.shape[0]
    own_ref[...] = mixed[:rows]
    other_ref[...] = mixed[rows:].astype(jnp.bfloat16)


def mix(mixes, parts):
    shape = (mixes.shape[0] // 2, parts[0].shape[1])
    return pl.pallas_call(
        mix_kernel,
        out_shape=[
            jax.ShapeDtypeStruct(shape, jnp.float32),
            jax.ShapeDtypeStruct(shape, jnp.bfloat16),
        ],
        compiler_params=pltpu.CompilerParams(vmem_limit_bytes=VMEM_LIMIT),
        name="mix",
    )(mixes, *parts)


def swiglu_kernel(count, after, scale, *refs):
    parts = refs[:count]
    gate_ref, up_ref, down_ref = refs[count : count + 3]
    outs, (held, total) = refs[count + 3 + after : -2], refs[-2:]
    step = pl.program_id(0)
    size = parts[0].shape[0]

    @pl.when(step == 0)
    def _():
        for o, part in enumerate(parts):
            held[o * size : (o + 1) * size, :] = part[...]
        if scale:
            total[...] = scale * held[...].astype(jnp.float32)
        else:
            total[...] = jnp.zeros_like(total)

    rows = held[...]
    gated = jnp.dot(rows, gate_ref[...], preferred_element_type=jnp.float32)
    lifted = jnp.dot(rows, up_ref[...], preferred_element_type=jnp.float32)
    inner = (gated / (1.0 + jnp.exp(-gated)) * lifted).astype(jnp.bfloat16)
    total[...] += jnp.dot(inner, down_ref[...], preferred_element_type=jnp.float32)

    @pl.when(step == pl.num_programs(0) - 1)
    def _():
        for o, out in enumerate(outs):
            out[...] = total[o * size : (o + 1) * size, :].astype(out.dtype)


def swiglu(parts, gate_mat, up_mat, down_mat, kind, after=(), scale=0.0):
    count, (size, width) = len(parts), parts[0].shape
    hidden = gate_mat.shape[-1]
    block = hidden
    lead = (None,) * (gate_mat.ndim - 2)
    zero = (0,) * len(lead)
    whole = pl.BlockSpec((size, width), lambda i: (0, 0))
    return pl.pallas_call(
        functools.partial(swiglu_kernel, count, len(after), scale),
        grid=(hidden // block,),
        in_specs=[whole] * count
        + [pl.BlockSpec((*lead, width, block), lambda i: (*zero, 0, i))] * 2
        + [pl.BlockSpec((*lead, block, width), lambda i: (*zero, i, 0))]
        + [pl.BlockSpec(memory_space=pl.ANY)] * len(after),
        out_specs=[whole] * count,
        out_shape=[jax.ShapeDtypeStruct((size, width), kind)] * count,
        scratch_shapes=[
            pltpu.VMEM((count * size, width), jnp.bfloat16),
            pltpu.VMEM((count * size, width), jnp.float32),
        ],
        compiler_params=pltpu.CompilerParams(
            dimension_semantics=("arbitrary",), vmem_limit_bytes=VMEM_LIMIT
        ),
        name="swiglu",
    )(*parts, gate_mat, up_mat, down_mat, *after)


def finish_kernel(feed_ref, own_ref, core_ref, far_ref, gain_ref, bias_ref, out_ref):
    feed = feed_ref[...] + own_ref[...] + core_ref[...].astype(jnp.float32)
    feed = feed + far_ref[...].astype(jnp.float32)
    out_ref[...] = layer_norm(feed, gain_ref[...], bias_ref[...]).astype(jnp.bfloat16)


def finish(feed, *args):
    return pl.pallas_call(
        finish_kernel,
        out_shape=jax.ShapeDtypeStruct(feed.shape, jnp.bfloat16),
        compiler_params=pltpu.CompilerParams(vmem_limit_bytes=VMEM_LIMIT),
        name="finish",
    )(feed, *args)


def depth_of(seq_devices):
    bits = seq_devices.bit_length() - 1
    return 1 << ((bits + 1) // 2)


def send(values, dsp, ddp):
    count, side = lax.axis_size("sp"), lax.axis_size("dp")
    pairs = [
        (i * side + k, (i ^ dsp) * side + (k ^ ddp)) for i in range(count) for k in range(side)
    ]
    return lax.ppermute(values, ("sp", "dp"), pairs)


def attention_kernel(blocks, after, latent_width, here_ref, query_ref, table_ref, *refs):
    packed_refs = refs[:blocks]
    (
        up_ref,
        hidden_ref,
        attn_gain_ref,
        gain_ref,
        bias_ref,
        out_proj_ref,
    ) = refs[blocks : blocks + 6]
    out_ref, latent, rope, attended, out_proj, sem = refs[blocks + 6 + after :]
    step = pl.program_id(0)
    steps = pl.num_programs(0)
    rows = hidden_ref.shape[0]
    load = pltpu.make_async_copy(out_proj_ref, out_proj, sem)

    @pl.when(step == 0)
    def _():
        load.start()
        for j in range(blocks):
            latent[j * rows : (j + 1) * rows, :] = packed_refs[j][:, :latent_width]
            rope[j * rows : (j + 1) * rows, :] = packed_refs[j][:, latent_width:]

    key_values = jnp.dot(latent[...], up_ref[...], preferred_element_type=jnp.float32).astype(
        jnp.bfloat16
    )
    here = here_ref[0]
    width = PLAIN_HEAD_WIDTH + VALUE_HEAD_WIDTH
    key_width = PLAIN_HEAD_WIDTH + QK_ROPE
    factor = math.log2(math.e) / math.sqrt(key_width)
    causal = lax.broadcasted_iota(jnp.int32, (rows, rows), 1) <= lax.broadcasted_iota(
        jnp.int32, (rows, rows), 0
    )
    lane = lax.broadcasted_iota(jnp.int32, (rows, LANES), 1)
    query = query_ref[...].astype(jnp.float32)
    outs = []
    for head in range(HEADS_STEP):
        tile, offset = divmod(head * key_width, LANES)
        mine = query[:, tile * LANES : (tile + 1) * LANES]
        if offset:
            mine = pltpu.roll(mine, LANES - offset, 1)
        if offset + key_width > LANES:
            after = query[:, (tile + 1) * LANES : (tile + 2) * LANES]
            mine = jnp.where(lane < LANES - offset, mine, pltpu.roll(after, LANES - offset, 1))
        query_full = jnp.concatenate(
            [jnp.where(lane < PLAIN_HEAD_WIDTH, mine, 0.0), turned(mine, table_ref[...])], axis=1
        ).astype(jnp.bfloat16)
        head_kv = key_values[:, head * width : (head + 1) * width]
        key_full = jnp.concatenate([head_kv, rope[...]], axis=1)
        scores = lax.dot_general(
            query_full,
            key_full,
            (((1,), (1,)), ((), ())),
            preferred_element_type=jnp.float32,
        )
        parts = [jnp.where(causal, scores[:, :rows], MASKED)]
        for j in range(1, blocks):
            seen = (here ^ j) < here
            parts.append(jnp.where(seen, scores[:, j * rows : (j + 1) * rows], MASKED))
        scores = jnp.concatenate(parts, axis=1)
        row_max = jnp.max(scores, axis=1, keepdims=True)
        weights = jnp.exp2((scores - row_max) * factor)
        total = jnp.sum(weights, axis=1, keepdims=True)
        summed = jnp.dot(
            weights.astype(jnp.bfloat16), head_kv, preferred_element_type=jnp.float32
        )
        outs.append(summed / total)
    for pair in range(HEADS_STEP // 2):
        left, right = outs[2 * pair : 2 * pair + 2]
        attended[step * (HEADS_STEP // 2) + pair] = jnp.where(
            lane < VALUE_HEAD_WIDTH, pltpu.roll(left, VALUE_HEAD_WIDTH, 1), right
        ).astype(jnp.bfloat16)

    @pl.when(step == steps - 1)
    def _():
        load.wait()
        whole = jnp.concatenate([attended[i] for i in range(attended.shape[0])], axis=1)
        normed = rms_scaled(whole, attn_gain_ref[...]).astype(jnp.bfloat16)
        mixed = jnp.dot(normed, out_proj[...], preferred_element_type=jnp.float32)
        out_ref[...] = layer_norm(
            ALPHA * hidden_ref[...].astype(jnp.float32) + mixed, gain_ref[...], bias_ref[...]
        ).astype(jnp.bfloat16)


def attention_layer(
    here, queries, table, packed, latent_up_weight, hidden, attn_gain, out_proj, gain, bias, after=()
):
    blocks = len(packed)
    rows = queries.shape[0]
    latent_width = latent_up_weight.shape[0]
    width = PLAIN_HEAD_WIDTH + VALUE_HEAD_WIDTH
    heads = latent_up_weight.shape[1] // width
    whole = lambda array: pl.BlockSpec(array.shape, lambda i, here: (0,) * array.ndim)
    return pl.pallas_call(
        functools.partial(attention_kernel, blocks, len(after), latent_width),
        grid_spec=pltpu.PrefetchScalarGridSpec(
            num_scalar_prefetch=1,
            grid=(heads // HEADS_STEP,),
            in_specs=[
                pl.BlockSpec(
                    (rows, HEADS_STEP * (PLAIN_HEAD_WIDTH + QK_ROPE)), lambda i, here: (0, i)
                ),
                pl.BlockSpec((rows, LANES), lambda i, here: (here[0], 0)),
                *[whole(p) for p in packed],
                pl.BlockSpec((latent_width, HEADS_STEP * width), lambda i, here: (0, i)),
                whole(hidden),
                whole(attn_gain),
                whole(gain),
                whole(bias),
                pl.BlockSpec(memory_space=pltpu.HBM),
                *[pl.BlockSpec(memory_space=pl.ANY)] * len(after),
            ],
            out_specs=pl.BlockSpec(hidden.shape, lambda i, here: (0, 0)),
            scratch_shapes=[
                pltpu.VMEM((blocks * rows, latent_width), jnp.bfloat16),
                pltpu.VMEM((blocks * rows, LANES), jnp.bfloat16),
                pltpu.VMEM((heads // 2, rows, 2 * VALUE_HEAD_WIDTH), jnp.bfloat16),
                pltpu.VMEM(out_proj.shape, jnp.bfloat16),
                pltpu.SemaphoreType.DMA,
            ],
        ),
        out_shape=jax.ShapeDtypeStruct(hidden.shape, jnp.bfloat16),
        compiler_params=pltpu.CompilerParams(
            dimension_semantics=("arbitrary",), vmem_limit_bytes=VMEM_WIDE
        ),
        name="attention_layer",
    )(here, queries, table, *packed, latent_up_weight, hidden, attn_gain, gain, bias, out_proj, *after)


def per_device(
    hidden_in,
    queries,
    key_value_latent,
    keys_rope,
    latent_norm_gain,
    latent_up_weight,
    attn_gain,
    out_proj,
    norm1_gain,
    norm1_bias,
    expert_ids,
    route_weights,
    gate_proj,
    up_proj,
    down_proj,
    shared_gate,
    shared_up,
    shared_down,
    norm2_gain,
    norm2_bias,
):
    seq_devices = lax.axis_size("sp")
    depth = depth_of(seq_devices)
    across = seq_devices // depth
    tok_rows = hidden_in.shape[1]
    here = lax.axis_index("sp")

    index = here.reshape(1).astype(jnp.int32)
    table = rotation_table(seq_devices * tok_rows, QK_ROPE)

    packed = pack(
        index,
        key_value_latent[0],
        latent_norm_gain[None],
        keys_rope[0].T,
        expert_ids[0].T,
        route_weights[0].T,
        table,
    )
    gathered = [packed] + [None] * (seq_devices - 1)
    for dz in range(depth - 1, 0, -1):
        gathered[dz * across] = send(packed, dz * across, 0)
    for dy in range(1, across):
        gathered[dy] = send(packed, dy, 0)
    for dz in range(1, depth):
        for dy in range(1, across):
            gathered[dz * across + dy] = send(gathered[dz * across], dy, 0)

    side_devices = lax.axis_size("dp")
    group = seq_devices * side_devices
    capacity = (tok_rows * TOP_K * 3 + 2 * group - 1) // (2 * group)
    capacity = -(-capacity // 8) * 8
    half = seq_devices // 2
    offsets = [(d, k) for d in range(half) for k in range(0, side_devices, 2)]
    offsets = offsets[:1] + offsets[:0:-1]
    peers = len(offsets)
    slots = peers * 2 * capacity
    column = lax.axis_index("dp")
    wanted = jnp.stack([(here ^ d) * side_devices + (column ^ k) for d, k in offsets]).astype(
        jnp.float32
    )
    order = jnp.arange(tok_rows)
    before = (order[:, None] > order[None, :]).astype(jnp.bfloat16)
    same = jnp.eye(2, dtype=jnp.bool_)
    start = key_value_latent.shape[2] + TAG_LANE

    def routes(block):
        tags = block[:, start : start + 2 * TOP_K]
        tags = jnp.stack([tags, send(tags, 0, 1)]).astype(jnp.float32)
        named = tags[..., :TOP_K, None] == wanted
        member = jnp.any(named, axis=2)
        share = jnp.sum(jnp.where(named, tags[..., TOP_K:, None], 0.0), axis=2)
        slot = jnp.einsum(
            "ts,bsp->btp", before, member.astype(jnp.bfloat16), preferred_element_type=jnp.float32
        ).astype(jnp.int32)
        filled = member[..., None] & (slot[..., None] == jnp.arange(capacity, dtype=jnp.int32))
        picks = (
            (jnp.transpose(filled, (2, 0, 3, 1))[:, :, :, None, :] & same[:, None, :, None])
            .reshape(slots, 2 * tok_rows)
            .astype(jnp.bfloat16)
        )
        gated = jnp.where(filled, share[..., None], 0.0)
        mixes = (
            jnp.where(same[:, None, None, :, None], gated[:, :, :, None, :], 0.0)
            .reshape(2 * tok_rows, slots)
            .astype(jnp.bfloat16)
        )
        return picks, mixes

    near_picks, near_mixes = routes(packed)
    far_picks, far_mixes = routes(gathered[half])

    first = attention_layer(
        index,
        queries[0],
        table,
        gathered,
        latent_up_weight,
        hidden_in[0],
        attn_gain[None],
        out_proj,
        norm1_gain[None],
        norm1_bias[None],
        (near_picks, far_picks, near_mixes, far_mixes),
    )

    def exchange(parts):
        outs = [parts[0]]
        for o in range(1, peers):
            outs.append(send(parts[o], *offsets[o]))
        return outs

    experts = functools.partial(swiglu, gate_mat=gate_proj, up_mat=up_proj, down_mat=down_proj)
    far = send(first, half, 0)
    sibling = send(first, 0, 1)
    near_sent = pick(near_picks, first, sibling, peers)
    near = exchange(near_sent)
    (feed,) = swiglu(
        [first], shared_gate, shared_up, shared_down, jnp.float32, near_sent[:1], ALPHA
    )
    far_sibling = send(far, 0, 1)
    far_sent = pick(far_picks, far, far_sibling, peers)
    away = exchange(far_sent)
    near_done = experts(near, kind=jnp.bfloat16, after=(far_sent[1], feed))
    away_done = experts(away, kind=jnp.bfloat16, after=near_done[1:2])
    away_back = exchange(away_done)
    near_back = exchange(near_done)
    far_own, far_core = mix(far_mixes, away_back)
    far_core = send(far_core, 0, 1)
    far_sum = (far_own + far_core.astype(jnp.float32)).astype(jnp.bfloat16)
    far_sum = send(far_sum, half, 0)
    own, core = mix(near_mixes, near_back)
    core = send(core, 0, 1)
    result = finish(feed, own, core, far_sum, norm2_gain[None], norm2_bias[None])
    return result.reshape(1, tok_rows, D)


def solution(mesh):
    in_specs = (
        P("dp", "sp", None),
        P("dp", "sp", None),
        P("dp", "sp", None),
        P("dp", "sp", None),
        P(),
        P(),
        P(),
        P(),
        P(),
        P(),
        P("dp", "sp", None),
        P("dp", "sp", None),
        P(("sp", "dp"), None, None),
        P(("sp", "dp"), None, None),
        P(("sp", "dp"), None, None),
        P(),
        P(),
        P(),
        P(),
        P(),
    )
    out_specs = P("dp", "sp", None)
    return jax.shard_map(
        per_device, mesh=mesh, in_specs=in_specs, out_specs=out_specs, check_vma=False
    )
```
